512 devices in a mesh: fs: 64 (over z, y), rep: 4 (over x), tp: 2 (over core).
Axes of the slice: x: 4, y: 8, z: 8, core: 2. Of those that a mesh axis runs over, the one named last changes fastest.
Arguments:
- saved_in: bfloat16 [65536, 4096], P(('fs', 'rep', 'tp')), may hold values from -6 to 6
- out_cot: bfloat16 [65536, 4096], P(('fs', 'rep', 'tp')), may hold values from -0.0234375 to 0.0234375
- value_cot: bfloat16 [65536, 2048], P(('fs', 'rep'), 'tp'), may hold values from -0.0234375 to 0.0234375
- mixed_out: bfloat16 [65536, 2048], P(('fs', 'rep'), 'tp'), may hold values from -6 to 6
- value_factor: bfloat16 [4096, 512], P('fs'), may hold values from -0.09375 to 0.09375
- out_factor: bfloat16 [4096, 512], P('fs'), may hold values from -0.09375 to 0.09375
- value_weight: float32 [4096, 2048], P('fs', 'tp'), may hold values from -0.09375 to 0.09375
- out_weight: float32 [2048, 4096], P('tp', 'fs'), may hold values from -0.125 to 0.125
- value_first: float32 [512, 2048], P('fs', 'tp'), may hold values from -6 to 6
- value_second: float32 [512, 2048], P('fs', 'tp'), may hold values from 0.25 to 4
- out_first: float32 [512, 2048], P('fs', 'tp'), may hold values from -6 to 6
- out_second: float32 [512, 2048], P('fs', 'tp'), may hold values from 0.25 to 4
Outputs:
- value_weight_new: float32 [4096, 2048], P('fs', 'tp')
- value_weight_copy: bfloat16 [4096, 2048], P('fs', 'tp')
- out_weight_new: float32 [2048, 4096], P('tp', 'fs')
- out_weight_copy: bfloat16 [2048, 4096], P('tp', 'fs')
- value_first_new: float32 [512, 2048], P('fs', 'tp')
- value_second_new: float32 [512, 2048], P('fs', 'tp')
- out_first_new: float32 [512, 2048], P('fs', 'tp')
- out_second_new: float32 [512, 2048], P('fs', 'tp')
- value_step: float32 [512, 2048], P('fs', 'tp')
- out_step: float32 [512, 2048], P('fs', 'tp')
The draws below stay inside these ranges and needn't reach their ends.
All inputs are finite; a program needn't handle non-finite values.
Results may differ from the reference program's by a relative error of at most 0.005.
Values may be sent and summed in bfloat16 or wider, within the bound.
A program may use at most 64 MiB of HBM per device.

```python
import math
import jax
import jax.numpy as jnp

MODEL_DIM = 4096
CHANNELS = 2048
RANK = 512
TOKENS = 65536


def steps_of(stream_key, shape, pieces, least, largest):
    def one(position, blocks):
        draws = jax.random.uniform(jax.random.fold_in(jax.random.fold_in(stream_key, 6), position), (blocks,), jnp.float32, least / len(pieces), largest / len(pieces))
        return jnp.repeat(jnp.exp(draws), shape[position] // blocks).reshape((-1,) + (1,) * (len(shape) - position - 1))

    level = one(*pieces[0])
    for cut in pieces[1:]:
        level = level * one(*cut)
    return level


def bell_draw(rng, extent, scale, most, split=(), held_as=jnp.bfloat16):
    factor_of = steps_of(rng, extent, split, -0.22, 0.18) if split else 1.0
    drawn = jax.random.normal(rng, extent, jnp.float32) * scale * factor_of
    return jnp.minimum(jnp.maximum(drawn, -most), most).astype(held_as)


def setup_inputs(seed: int = 0) -> dict:
    arg_keys = jax.random.split(jax.random.key(seed), 13)
    return {
        "saved_in": bell_draw(arg_keys[0], (TOKENS, MODEL_DIM), 1.0, 6.0, ((0, 512),)),
        "out_cot": bell_draw(arg_keys[1], (TOKENS, MODEL_DIM), (TOKENS ** -0.5), 0.0234375, ((0, 512),)),
        "value_cot": bell_draw(arg_keys[2], (TOKENS, CHANNELS), (TOKENS ** -0.5), 0.0234375, ((0, 256), (1, 2))),
        "mixed_out": bell_draw(arg_keys[3], (TOKENS, CHANNELS), 1.0, 6.0, ((0, 256), (1, 2))),
        "value_factor": bell_draw(arg_keys[4], (MODEL_DIM, RANK), MODEL_DIM ** -0.5, 0.09375, ((0, 64),)),
        "out_factor": bell_draw(arg_keys[5], (MODEL_DIM, RANK), MODEL_DIM ** -0.5, 0.09375, ((0, 64),)),
        "value_weight": bell_draw(arg_keys[6], (MODEL_DIM, CHANNELS), MODEL_DIM ** -0.5, 0.09375, ((0, 64), (1, 2)), jnp.float32),
        "out_weight": bell_draw(arg_keys[7], (CHANNELS, MODEL_DIM), CHANNELS ** -0.5, 0.125, ((0, 2), (1, 64)), jnp.float32),
        "value_first": bell_draw(arg_keys[8], (RANK, CHANNELS), 1.0, 6.0, ((0, 64), (1, 2)), jnp.float32),
        "value_second": jnp.clip(jnp.exp(math.log(4.0) - 2.7725887 * jax.random.uniform(arg_keys[9], (RANK, CHANNELS), jnp.float32) ** steps_of(arg_keys[9], (RANK, CHANNELS), ((0, 64), (1, 2)), -0.2, 0.2)), 0.25, 4.0),
        "out_first": bell_draw(arg_keys[10], (RANK, CHANNELS), 1.0, 6.0, ((0, 64), (1, 2)), jnp.float32),
        "out_second": jnp.clip(jnp.exp(math.log(4.0) - 2.7725887 * jax.random.uniform(arg_keys[11], (RANK, CHANNELS), jnp.float32) ** steps_of(arg_keys[11], (RANK, CHANNELS), ((0, 64), (1, 2)), -0.2, 0.2)), 0.25, 4.0),
    }


beta_first = 0.8
beta_second = 0.9
step_rate = 0.05
clip_level = 0.5

def adapt(grad, first, second):
    new_first = beta_first * first + (1.0 - beta_first) * grad
    new_second = beta_second * second + (1.0 - beta_second) * grad * grad
    lowered = (new_first / jnp.sqrt(new_second)).astype(jnp.bfloat16)
    return (new_first, new_second, lowered)

def reference(saved_in, out_cot, value_cot, mixed_out, value_factor, out_factor, value_weight, out_weight, value_first, value_second, out_first, out_second):
    proj_in = jnp.dot(saved_in, value_factor, preferred_element_type=jnp.float32).astype(jnp.bfloat16)
    proj_cot = jnp.dot(out_cot, out_factor, preferred_element_type=jnp.float32).astype(jnp.bfloat16)
    grad_value = jnp.dot(proj_in.T, value_cot, preferred_element_type=jnp.float32)
    grad_out = jnp.dot(proj_cot.T, mixed_out, preferred_element_type=jnp.float32)
    value_first_new, value_second_new, low_value = adapt(grad_value, value_first, value_second)
    out_first_new, out_second_new, low_out = adapt(grad_out, out_first, out_second)
    value_float = low_value.astype(jnp.float32)
    out_float = low_out.astype(jnp.float32)
    total = jnp.sum(value_float * value_float) + jnp.sum(out_float * out_float)
    spread = jnp.sqrt(total / (2.0 * RANK * CHANNELS))
    scale = clip_level / jnp.maximum(spread, clip_level)
    value_full = jnp.dot(value_factor, low_value, preferred_element_type=jnp.float32)
    out_full = jnp.dot(low_out.T, out_factor.T, preferred_element_type=jnp.float32)
    value_weight_new = value_weight - step_rate * scale * value_full
    out_weight_new = out_weight - step_rate * scale * out_full
    return (value_weight_new, value_weight_new.astype(jnp.bfloat16), out_weight_new, out_weight_new.astype(jnp.bfloat16), value_first_new, value_second_new, out_first_new, out_second_new, scale * value_float, scale * out_float)
```

```python
import jax
import jax.numpy as jnp
from jax import lax
from jax.experimental import pallas as pl
from jax.experimental.pallas import tpu as pltpu
from jax.sharding import Mesh
from jax.sharding import PartitionSpec as P

MESH = pl.DeviceIdType.MESH
FS = ("fs_0", "fs_1")
FS_REP_TP = ("fs_0", "fs_1", "rep", "tp")
FS_REP = ("fs_0", "fs_1", "rep")

beta_first = 0.8
beta_second = 0.9
step_rate = 0.05
clip_level = 0.5

SUBS = 2


def body(
    sizes,
    total_count,
    saved_in,
    out_cot,
    value_cot,
    mixed_out,
    value_factor,
    out_factor,
    value_weight,
    out_weight_t,
    value_first,
    value_second,
    out_first,
    out_second,
    vw_new,
    vw_copy,
    ow_new,
    ow_copy,
    vf_new,
    vs_new,
    of_new,
    os_new,
    v_step,
    o_step,
    factor,
    tokens,
    acc,
    cots,
    proj,
    grads,
    own_factor,
    weights,
    moments,
    send_1,
    recv_1,
    send_2,
    own_2,
    recv_2,
    recv_3,
    low,
    rows_low,
    product,
    squares,
    local_sem,
    tok_sem,
    ga_send,
    ga_recv,
    proj_sem,
    s1_send,
    s1_recv,
    s2_send,
    s2_recv,
    s3_send,
    s3_recv,
    e1_send,
    e1_recv,
    e2_send,
    e2_recv,
    xp_send,
    xp_recv,
    ss_send,
    ss_recv,
):
    nz, ny, nx = sizes
    z, y = lax.axis_index("fs_0"), lax.axis_index("fs_1")
    x, c = lax.axis_index("rep"), lax.axis_index("tp")
    shard = value_factor.shape[0]
    half = shard // 2
    mine = saved_in.shape[0]
    chans = value_cot.shape[1]
    quarter = chans // nx

    def at_z(d):
        return (lax.rem(z + d + nz, nz), y, x, c)

    def at_y(d):
        return (z, lax.rem(y + d + ny, ny), x, c)

    def at_x(d, core=0):
        return (z, y, lax.rem(x + d, nx), lax.rem(c + core, 2))

    pair = (z, y, x, 1 - c)

    peers = [at_z(d) for d in range(1, nz)] + [at_y(d) for d in range(1, ny)]
    peers += [at_x(d, k) for k in range(2) for d in range(nx) if (d, k) != (0, 0)]
    barrier = pltpu.get_barrier_semaphore()
    for peer in peers:
        pl.semaphore_signal(barrier, inc=1, device_id=peer, device_id_type=MESH)

    def local(src, dst, k):
        return pltpu.make_async_copy(src, dst, local_sem.at[k])

    def shard_rows(zi, yi, h):
        return pl.ds(pl.multiple_of((zi * ny + yi) * shard + h * half, half), half)

    own_rows = pl.ds(pl.multiple_of((z * ny + y) * shard, shard), shard)
    own_tokens = pl.ds(pl.multiple_of(c * mine, mine), mine)

    @pl.when(c == 0)
    def _():
        local(value_factor, factor.at[own_rows], 0).start()
        local(saved_in, tokens.at[own_tokens], 1).start()

    @pl.when(c == 1)
    def _():
        local(out_factor, factor.at[own_rows], 0).start()
        local(out_cot, tokens.at[own_tokens], 1).start()

    fetches = [
        local(value_cot, cots.at[0], 2),
        local(mixed_out, cots.at[1], 3),
        local(value_factor, own_factor.at[0], 4),
        local(out_factor, own_factor.at[1], 5),
        local(value_weight, weights.at[0], 6),
        local(out_weight_t, weights.at[1], 7),
        local(value_first, moments.at[0], 8),
        local(value_second, moments.at[1], 9),
        local(out_first, moments.at[2], 10),
        local(out_second, moments.at[3], 11),
    ]
    for fetch in fetches:
        fetch.start()
    pl.semaphore_wait(barrier, len(peers))

    def remote(src, dst, send_sem, recv_sem, to):
        return pltpu.make_async_remote_copy(
            src_ref=src,
            dst_ref=dst,
            send_sem=send_sem,
            recv_sem=recv_sem,
            device_id=to,
            device_id_type=MESH,
        )

    local(value_factor, factor.at[own_rows], 0).wait()

    swap_in = remote(saved_in, tokens.at[own_tokens], tok_sem.at[0], tok_sem.at[1], pair)
    swap_cot = remote(out_cot, tokens.at[own_tokens], tok_sem.at[0], tok_sem.at[1], pair)

    @pl.when(c == 0)
    def _():
        swap_cot.start()

    @pl.when(c == 1)
    def _():
        swap_in.start()

    def order(n):
        shifts = [0]
        for d in range(1, n // 2 + 1):
            shifts.append(-d)
            if d <= (n - 1) // 2:
                shifts.append(d)
        return shifts

    class Color:
        def __init__(self, h):
            self.h = h
            self.na, self.nb = (nz, ny) if h == 0 else (ny, nz)
            self.pa, self.pb = (z, y) if h == 0 else (y, z)
            self.to_a, self.to_b = (at_z, at_y) if h == 0 else (at_y, at_z)
            self.count = 0

        def chunk(self, da, db):
            ia = lax.rem(self.pa + da + self.na, self.na)
            ib = lax.rem(self.pb + db + self.nb, self.nb)
            zi, yi = (ia, ib) if self.h == 0 else (ib, ia)
            return factor.at[shard_rows(zi, yi, self.h)]

        def slot(self, da, db):
            return ga_recv.at[self.h, order(self.na).index(da) * self.nb + order(self.nb).index(db)]

        def send(self, da, db, to, slot):
            ref = self.chunk(da, db)
            remote(ref, ref, ga_send.at[self.h], slot, to).start()
            self.count += 1

        def wait(self, da, db):
            ref = self.chunk(da, db)
            remote(ref, ref, ga_send.at[self.h], self.slot(da, db), pair).wait_recv()

        def on_a(self, da):
            ups, downs = self.na // 2, (self.na - 1) // 2
            if da <= 0 and -da < ups:
                self.send(da, 0, self.to_a(1), self.slot(da - 1, 0))
            if da >= 0 and da < downs:
                self.send(da, 0, self.to_a(-1), self.slot(da + 1, 0))

        def on_b(self, da, db):
            ups, downs = self.nb // 2, (self.nb - 1) // 2
            if db <= 0 and -db < ups:
                self.send(da, db, self.to_b(1), self.slot(da, db - 1))
            if db >= 0 and db < downs:
                self.send(da, db, self.to_b(-1), self.slot(da, db + 1))

        def round(self, t):
            for da in order(self.na):
                if abs(da) == t:
                    if da != 0:
                        self.wait(da, 0)
                    self.on_a(da)
                    self.on_b(da, 0)
            for da in order(self.na):
                for db in order(self.nb):
                    if db != 0 and abs(da) + abs(db) == t:
                        self.wait(da, db)
                        self.on_b(da, db)

        def finish(self):
            ref = factor.at[pl.ds(0, self.count * half)]
            remote(ref, ref, ga_send.at[self.h], ga_recv.at[self.h, 0], pair).wait_send()

    colors = [Color(0), Color(1)]
    for t in range(nz // 2 + ny // 2 + 1):
        for color in colors:
            color.round(t)

    local(saved_in, tokens.at[own_tokens], 1).wait()
    swap_in.wait()

    width = min(512, factor.shape[0])
    acc[...] = jnp.zeros_like(acc)

    @pl.loop(0, factor.shape[0] // width)
    def _(k):
        at = pl.ds(pl.multiple_of(k * width, width), width)
        acc[...] += jnp.dot(tokens[:, at], factor[at, :], preferred_element_type=jnp.float32)

    proj[c] = acc[...].astype(jnp.bfloat16)
    swap_proj = remote(proj.at[c], proj.at[c], proj_sem.at[0], proj_sem.at[1], pair)
    swap_proj.start()
    for fetch in fetches:
        fetch.wait()

    cut = min(256, chans)

    def contract(which):
        left = proj[which]

        @pl.loop(0, chans // cut)
        def _(k):
            at = pl.ds(pl.multiple_of(k * cut, cut), cut)
            part = lax.dot_general(
                left,
                cots[which, :, at],
                (((0,), (0,)), ((), ())),
                preferred_element_type=jnp.float32,
            )
            grads[which, :, :, :, at] = part.reshape(nz, ny, 8, cut)

    contract(c)
    swap_proj.wait_recv()
    contract(1 - c)
    sent = [swap_proj]

    piece = chans // SUBS

    def of_dest(h, dest, sub):
        cols = pl.ds(sub * piece, piece)
        if h == 0:
            return grads[0, :, dest, :, cols].reshape(nz * 8, piece)
        return grads[1, dest, :, :, cols].reshape(ny * 8, piece)

    ring = [(ny, y, at_y, nz, z, at_z), (nz, z, at_z, ny, y, at_y)]

    def step_1(h, step, sub):
        n, pos, to, _, _, _ = ring[h]
        ups, downs = n // 2, (n - 1) // 2
        for way, hops, sign in ((0, ups, 1), (1, downs, -1)):
            if step >= hops:
                continue
            dest = lax.rem(pos + sign * (hops - step) + n, n)
            part = of_dest(h, dest, sub)
            if step > 0:
                wait_1(h, way, step - 1, sub)
                part = part + recv_1[h, way, step - 1, sub].astype(jnp.float32)
            send_1[h, way, step, sub] = part.astype(jnp.bfloat16)
            copy = remote(
                send_1.at[h, way, step, sub],
                recv_1.at[h, way, step, sub],
                s1_send.at[h, way, step, sub],
                s1_recv.at[h, way, step, sub],
                to(sign),
            )
            copy.start()
            sent.append(copy)

    def wait_1(h, way, step, sub):
        remote(
            send_1.at[h, way, step, sub],
            recv_1.at[h, way, step, sub],
            s1_send.at[h, way, step, sub],
            s1_recv.at[h, way, step, sub],
            pair,
        ).wait_recv()

    for step in range(max(nz, ny) // 2):
        for sub in range(SUBS):
            for h in range(2):
                step_1(h, step, sub)

    waits_2 = []
    for h in range(2):
        n, pos, _, m, other, to = ring[h]
        for sub in range(SUBS):
            part = of_dest(h, pos, sub)
            for way, hops in ((0, n // 2), (1, (n - 1) // 2)):
                if hops > 0:
                    wait_1(h, way, hops - 1, sub)
                    part = part + recv_1[h, way, hops - 1, sub].astype(jnp.float32)
            cols = pl.ds(sub * piece, piece)
            part = part.reshape(m, 8, piece)
            own_2[h, :, :, cols] = part
            send_2[h, :, :, cols] = part.astype(jnp.bfloat16)
        for d in range(1, m):
            copy = remote(
                send_2.at[h, lax.rem(other + d, m)],
                recv_2.at[h, d],
                s2_send.at[h, d],
                s2_recv.at[h, d],
                to(d),
            )
            copy.start()
            sent.append(copy)
            waits_2.append(copy)
    for copy in waits_2:
        copy.wait_recv()
    for h in range(2):
        _, _, _, m, other, _ = ring[h]
        part = own_2[h, other]
        for d in range(1, m):
            part = part + recv_2[h, d].astype(jnp.float32)
        recv_3[x, h] = part.astype(jnp.bfloat16)

    waits_3 = []
    for d in range(1, nx):
        copy = remote(recv_3.at[x], recv_3.at[x], s3_send.at[d], s3_recv.at[d], at_x(d))
        copy.start()
        sent.append(copy)
        waits_3.append(copy)
    for copy in waits_3:
        copy.wait_recv()

    for h, (first_new, second_new) in enumerate(((vf_new, vs_new), (of_new, os_new))):
        grad = recv_3[0, h].astype(jnp.float32)
        for k in range(1, nx):
            grad = grad + recv_3[k, h].astype(jnp.float32)
        new_first = beta_first * moments[2 * h] + (1.0 - beta_first) * grad
        new_second = beta_second * moments[2 * h + 1] + (1.0 - beta_second) * grad * grad
        first_new[...] = new_first
        second_new[...] = new_second
        low[h] = (new_first / jnp.sqrt(new_second)).astype(jnp.bfloat16)

    for h in range(2):
        rows_low[h, z, y] = low[h, :, pl.ds(pl.multiple_of(x * quarter, quarter), quarter)]

    waits = []
    for h in range(2):
        n, _, _, m, _, to = ring[h]
        for d in range(1, m):
            ref = rows_low.at[h, z, y]
            copy = remote(ref, ref, e1_send.at[h, d], e1_recv.at[h, d], to(d))
            copy.start()
            sent.append(copy)
            waits.append(copy)
    for copy in waits:
        copy.wait_recv()
    waits = []
    for h in range(2):
        n, _, to, _, _, _ = ring[h]
        for d in range(1, n):
            ref = rows_low.at[0, :, y] if h == 0 else rows_low.at[1, z]
            copy = remote(ref, ref, e2_send.at[h, d], e2_recv.at[h, d], to(d))
            copy.start()
            sent.append(copy)
            waits.append(copy)
    for copy in waits:
        copy.wait_recv()

    square = jnp.zeros((), jnp.float32)
    for h in range(2):
        whole = rows_low[h].reshape(nz * ny * 8, quarter)
        wide = whole.astype(jnp.float32)
        square = square + jnp.sum(wide * wide)
        product[x, h] = jnp.dot(
            own_factor[h], whole, preferred_element_type=jnp.float32
        ).astype(jnp.bfloat16)
    squares[x, c] = jnp.full(squares.shape[2:], square, jnp.float32)

    waits = []
    for k in range(2):
        for d in range(nx):
            if (d, k) == (0, 0):
                continue
            ref = squares.at[x, c]
            copy = remote(
                ref, ref, ss_send.at[k * nx + d], ss_recv.at[k * nx + d], at_x(d, k)
            )
            copy.start()
            sent.append(copy)
            waits.append(copy)
    for d in range(1, nx):
        copy = remote(product.at[x], product.at[x], xp_send.at[d], xp_recv.at[d], at_x(d))
        copy.start()
        sent.append(copy)
        waits.append(copy)
    for copy in waits:
        copy.wait_recv()

    total = squares[0, 0] + squares[0, 1]
    for k in range(1, nx):
        total = total + squares[k, 0] + squares[k, 1]
    spread = jnp.sqrt(total / total_count)
    scale = (clip_level / jnp.maximum(spread, clip_level))[0:1, 0:1]
    for h, (new, copied, step) in enumerate(
        ((vw_new, vw_copy, v_step), (ow_new, ow_copy, o_step))
    ):
        for k in range(nx):
            cols = pl.ds(k * quarter, quarter)
            fresh = weights[h, :, cols] - step_rate * scale * product[k, h].astype(jnp.float32)
            new[:, cols] = fresh
            copied[:, cols] = fresh.astype(jnp.bfloat16)
        step[...] = scale * low[h].astype(jnp.float32)

    for copy in sent:
        copy.wait_send()
    for color in colors:
        color.finish()


def fused(sizes, args):
    nz, ny, nx = sizes
    (saved_in, _, value_cot, _, value_factor, _, value_weight, _, value_first, _, _, _) = args
    shard, rank = value_factor.shape
    model = shard * nz * ny
    mine = saved_in.shape[0]
    chans = value_cot.shape[1]
    quarter = chans // nx
    f32, bf16 = jnp.float32, jnp.bfloat16
    big = max(nz, ny)
    steps = big // 2
    dma = pltpu.SemaphoreType.DMA
    weight = jax.ShapeDtypeStruct(value_weight.shape, f32)
    copied = jax.ShapeDtypeStruct(value_weight.shape, bf16)
    moment = jax.ShapeDtypeStruct(value_first.shape, f32)
    assert nz == ny

    def kernel(*refs):
        body(sizes, 2.0 * rank * 2 * chans, *refs)

    return pl.pallas_call(
        kernel,
        name="update",
        out_shape=(weight, copied, weight, copied) + (moment,) * 6,
        in_specs=[pl.BlockSpec(memory_space=pl.ANY)] * 12,
        out_specs=[pl.BlockSpec(memory_space=pltpu.VMEM)] * 10,
        scratch_shapes=[
            pltpu.VMEM((model, rank), bf16),
            pltpu.VMEM((2 * mine, model), bf16),
            pltpu.VMEM((2 * mine, rank), f32),
            pltpu.VMEM((2, 2 * mine, chans), bf16),
            pltpu.VMEM((2, 2 * mine, rank), bf16),
            pltpu.VMEM((2, nz, ny, 8, chans), f32),
            pltpu.VMEM((2, shard, rank), bf16),
            pltpu.VMEM((2, shard, chans), f32),
            pltpu.VMEM((4, 8, chans), f32),
            pltpu.VMEM((2, 2, steps, SUBS, big * 8, chans // SUBS), bf16),
            pltpu.VMEM((2, 2, steps, SUBS, big * 8, chans // SUBS), bf16),
            pltpu.VMEM((2, big, 8, chans), bf16),
            pltpu.VMEM((2, big, 8, chans), f32),
            pltpu.VMEM((2, big, 8, chans), bf16),
            pltpu.VMEM((nx, 2, 8, chans), bf16),
            pltpu.VMEM((2, 8, chans), bf16),
            pltpu.VMEM((2, nz, ny, 8, quarter), bf16),
            pltpu.VMEM((nx, 2, shard, quarter), bf16),
            pltpu.VMEM((nx, 2, 8, 128), f32),
            dma((12,)),
            dma((2,)),
            dma((2,)),
            dma((2, nz * ny)),
            dma((2,)),
            dma((2, 2, steps, SUBS)),
            dma((2, 2, steps, SUBS)),
            dma((2, big)),
            dma((2, big)),
            dma((nx,)),
            dma((nx,)),
            dma((2, big)),
            dma((2, big)),
            dma((2, big)),
            dma((2, big)),
            dma((nx,)),
            dma((nx,)),
            dma((2 * nx,)),
            dma((2 * nx,)),
        ],
        compiler_params=pltpu.CompilerParams(
            collective_id=0, has_side_effects=True, vmem_limit_bytes=56 * 2**20
        ),
    )(*args)


def solution(mesh):
    side = {256: 16, 64: 8, 16: 4, 4: 2}[mesh.shape["fs"]]
    sizes = (side, side, mesh.shape["rep"])
    torus = Mesh(
        mesh.devices.reshape(side, side, mesh.shape["rep"], mesh.shape["tp"]),
        ("fs_0", "fs_1", "rep", "tp"),
    )

    def shards(*args):
        args = list(args)
        args[7] = args[7].T
        outs = list(fused(sizes, args))
        outs[2], outs[3] = outs[2].T, outs[3].T
        return tuple(outs)

    placed = (
        P(FS_REP_TP, None),
        P(FS_REP_TP, None),
        P(FS_REP, "tp"),
        P(FS_REP, "tp"),
        P(FS, None),
        P(FS, None),
        P(FS, "tp"),
        P("tp", FS),
        P(FS, "tp"),
        P(FS, "tp"),
        P(FS, "tp"),
        P(FS, "tp"),
    )
    return jax.shard_map(
        shards,
        mesh=torus,
        in_specs=placed,
        out_specs=(P(FS, "tp"), P(FS, "tp"), P("tp", FS), P("tp", FS)) + (P(FS, "tp"),) * 6,
        check_vma=False,
    )
```
